32 devices in a mesh: sp: 8 (over z, x), tp: 4 (over y, core).
Axes of the slice: x: 2, y: 2, z: 4, core: 2. Of those that a mesh axis runs over, the one named last changes fastest.
Arguments:
- moe_input: bfloat16 [1536, 2048], P('sp'), may hold values from -6 to 6
- out_grad: bfloat16 [1536, 2048], P('sp', 'tp'), may hold values from -6 to 6
- expert_ids: int32 [1536, 2], P('sp'), may hold values from 0 to 7, all different within a row; in each aligned block of 192 rows (0 to 191, 192 to 383, ...) at most 60 rows name the same one
- expert_weights: float32 [1536, 2], P('sp'), may hold values from 0.1 to 0.9
- w_gate: bfloat16 [8, 2048, 2048], P('sp', None, 'tp'), may hold values from -0.125 to 0.125
- w_up: bfloat16 [8, 2048, 2048], P('sp', None, 'tp'), may hold values from -0.125 to 0.125
- w_down: bfloat16 [8, 2048, 2048], P('sp', 'tp'), may hold values from -0.125 to 0.125
- out_proj: bfloat16 [1536, 2048], P('tp'), may hold values from -0.15625 to 0.15625
- retained: bfloat16 [1536, 1536], P('sp', 'tp'), may hold values from -6 to 6
- queries: bfloat16 [1536, 768], P('sp', 'tp'), may hold values from -6 to 6
- keys: bfloat16 [1536, 768], P('sp', 'tp'), may hold values from -0.86328125 to 0.86328125
- values: bfloat16 [1536, 1536], P('sp', 'tp'), may hold values from -6 to 6
- log_decay: float32 [1536, 16], P('sp', 'tp'), may hold values from -1 to 0
- incoming_state: float32 [8, 16, 48, 96], P('sp', 'tp'), may hold values from -6 to 6
Outputs:
- w_gate_grad: bfloat16 [8, 2048, 2048], P('sp', None, 'tp')
- w_up_grad: bfloat16 [8, 2048, 2048], P('sp', None, 'tp')
- w_down_grad: bfloat16 [8, 2048, 2048], P('sp', 'tp')
- out_proj_grad: float32 [2048, 1536], P('sp', 'tp')
- query_grad: bfloat16 [1536, 768], P('sp', 'tp')
- key_grad: bfloat16 [1536, 768], P('sp', 'tp')
- value_grad: bfloat16 [1536, 1536], P('sp', 'tp')
The draws below stay inside these ranges and needn't reach their ends.
Inputs may be any that keep to these rules, and one draw needn't show every extreme that they name: `expert_ids`: in each aligned block of 192 positions no expert is named by more than 60 of the block's assignments, a bound that some block reaches.
All inputs are finite; a program needn't handle non-finite values.
Results may differ from the reference program's by a relative error of at most 0.02.
Values may be sent and summed in bfloat16 or wider, within the bound.
A program may use at most 64 MiB of HBM per device.

```python
import math
import jax
import jax.numpy as jnp
import numpy as np
from jax import lax

D = 2048
RETENTION_HEADS = 16
KEY_DIM = 48
VALUE_DIM = 96
FF = 2048
TOK_DEV = 192
SEQUENCE_TOKENS = 1536
EXPERTS = 8
CAP = 60
RET_WIDTH = 1536
KEY_WIDTH = 768
N_SP = 8
N_TP = 4


def draw_log_decay(key, part):
    keys = jax.random.split(jax.random.fold_in(key, 17), 7)
    slow_share = 0.5
    slow = jax.random.uniform(keys[0], (RETENTION_HEADS,), jnp.float32) < slow_share
    slow_rate = jnp.exp(jax.random.uniform(keys[1], (RETENTION_HEADS,), jnp.float32, jnp.log(0.1), jnp.log(0.6))) / SEQUENCE_TOKENS
    fast_rate = jax.random.uniform(keys[2], (RETENTION_HEADS,), jnp.float32, 1.0 / 50.0, 1.0 / 30.0)
    decay_rate = jnp.where(slow, slow_rate, fast_rate)
    block_multiplier = jnp.repeat(jax.random.uniform(keys[3], (SEQUENCE_TOKENS // TOK_DEV,), jnp.float32, 0.5, 1.6), TOK_DEV)
    coarse_estimate = jax.random.uniform(keys[4], (SEQUENCE_TOKENS, 1), jnp.float32, 0.5, 1.5)
    spike_position = jax.random.randint(keys[5], (3,), 0, SEQUENCE_TOKENS)
    spike_mask = jnp.any(jnp.arange(SEQUENCE_TOKENS)[:, None] == spike_position[None, :], axis=1).astype(jnp.float32)
    spike_length = jax.random.uniform(keys[6], (RETENTION_HEADS,), jnp.float32, 0.22, 0.51)
    return -(decay_rate[None, :] * block_multiplier[:, None] * coarse_estimate) - spike_mask[:, None] * spike_length[None, :]


def raised(drawn, rng, source, target, blocks, factor):
    owner, partner = [(jnp.arange(drawn.shape[axis_at]) // (drawn.shape[axis_at] // blocks)).reshape([-1 if axis == axis_at else 1 for axis in range(drawn.ndim)]) for axis_at in (source, target)]
    chosen = jax.random.permutation(rng, blocks)[partner]
    strong = (owner == chosen) | (owner == (partner + blocks // 2) % blocks)
    return jnp.where(strong, factor * drawn, drawn)


def block_scale(key, shape, pieces, smallest, high):
    def one(position, blocks):
        heights = jax.random.uniform(jax.random.fold_in(jax.random.fold_in(key, 6), position), (blocks,), jnp.float32, smallest / len(pieces), high / len(pieces))
        return jnp.repeat(jnp.exp(heights), shape[position] // blocks).reshape((-1,) + (1,) * (len(shape) - position - 1))

    gain = one(*pieces[0])
    for cut in pieces[1:]:
        gain = gain * one(*cut)
    return gain


def deal_out(rng, own, number, rows, number_of, top, bound, slope):
    sequence = jax.random.permutation(rng, number_of)
    crowded, usual = load_shares(number_of, rows * top, bound, slope, True), load_shares(number_of, rows * top, bound, slope, False)
    places = jnp.arange(number_of)

    def named(tallies, rotation):
        used = int((tallies > 0).sum())
        fixed = max(1, used // 4)
        moved = fixed + (places - fixed + rotation * (used - fixed)) % max(1, number_of - fixed)
        return jnp.zeros((number_of,), jnp.int32).at[sequence[jnp.where(places < fixed, places, moved)]].set(jnp.asarray(tallies, jnp.int32))

    tallies = jnp.where(number % 4 == 0, named(crowded, number // 4), named(usual, number - number // 4 - 1))
    mixed = jax.random.permutation(jax.random.fold_in(own, 3), number_of)
    giver, receiver = mixed[0:number_of // 2 * 2:2], mixed[1:number_of // 2 * 2:2]
    slack = jnp.minimum(tallies[giver] - 1, bound - tallies[receiver]) // 2
    slack = jnp.where((giver == sequence[0]) | (receiver == sequence[0]) | (tallies[receiver] == 0), 0, jnp.maximum(slack, 0))
    moved = jax.random.randint(jax.random.fold_in(own, 4), (number_of // 2,), 0, 1 << 20) % (slack + 1)
    tallies = tallies.at[giver].add(-moved).at[receiver].add(moved)
    items = jnp.searchsorted(jnp.cumsum(tallies), jnp.arange(rows * top), side="right").astype(jnp.int32)
    grid = items.reshape(top, rows).T
    grid = grid[jax.random.permutation(jax.random.fold_in(own, 1), rows)]
    rotation = jax.random.randint(jax.random.fold_in(own, 2), (rows, 1), 0, top)
    return jnp.take_along_axis(grid, (jnp.arange(top)[None, :] + rotation) % top, axis=1)


def load_shares(number_of, total, reach, lean, full):
    loads = [(1 << 20) // math.isqrt(grade ** lean) + 1 for grade in range(1, number_of + 1)]
    largest = reach if full else min(reach, max(-(-total // number_of), total * loads[0] // sum(loads)))
    least = 1 if total - largest >= number_of - 1 else 0
    given, spare = [largest] + [least] * (number_of - 1), total - largest - least * (number_of - 1)
    while spare > 0:
        free = [i for i in range(1, number_of) if given[i] < largest] or [i for i in range(1, number_of) if given[i] < reach]
        pool, left = sum([loads[i] for i in free]), spare
        for i in free:
            addition = min(reach - given[i], max(1, left * loads[i] // pool), spare)
            given[i] = given[i] + addition
            spare = spare - addition
    return np.array(given)


def normal_values(key, dims, deviation, bound, cuts=(), kind=jnp.bfloat16):
    drawn = deviation * jax.random.normal(key, dims, jnp.float32)
    if cuts:
        drawn = drawn * block_scale(key, dims, cuts, -0.22, 0.18)
    return jnp.clip(drawn, -bound, bound).astype(kind)


def gaussian_with(key, shape, deviation, reach, cuts, heavy, kind=jnp.bfloat16):
    drawn = deviation * jax.random.normal(key, shape, jnp.float32)
    if cuts:
        drawn = drawn * block_scale(key, shape, cuts, -0.22, 0.18)
    return jnp.clip(raised(drawn, jax.random.fold_in(key, 3), *heavy), -reach, reach).astype(kind)


def setup_inputs(seed: int = 0) -> dict:
    key_list = jax.random.split(jax.random.key(seed), 15)
    moe_input = normal_values(key_list[0], (SEQUENCE_TOKENS, D), 1.0, 6.0, ((0, 8),))
    out_grad = gaussian_with(key_list[1], (SEQUENCE_TOKENS, D), 1.0, 6.0, ((0, 8), (1, 4)), (0, 1, 8, 2.0))
    expert_ids_keys = jax.random.split(jax.random.fold_in(key_list[2], 1), SEQUENCE_TOKENS // TOK_DEV)
    expert_ids_turns = jax.random.permutation(jax.random.fold_in(key_list[2], 3), SEQUENCE_TOKENS // TOK_DEV)
    expert_ids = jax.vmap(lambda own, number: deal_out(jax.random.fold_in(key_list[2], 2), own, number, TOK_DEV, EXPERTS, 2, CAP, 1))(expert_ids_keys, expert_ids_turns).reshape((SEQUENCE_TOKENS, 2))
    expert_weights = jnp.clip(0.1 + 0.79999997 * jax.random.uniform(key_list[3], (SEQUENCE_TOKENS, 2), jnp.float32) ** block_scale(key_list[3], (SEQUENCE_TOKENS, 2), ((0, 8),), -0.2, 0.2), 0.1, 0.9)
    w_gate = normal_values(key_list[4], (EXPERTS, D, FF), D ** -0.5, 0.125, ((0, 8), (2, 4)))
    w_up = normal_values(key_list[5], (EXPERTS, D, FF), D ** -0.5, 0.125, ((0, 8), (2, 4)))
    w_down = normal_values(key_list[6], (EXPERTS, FF, D), FF ** -0.5, 0.125, ((0, 8), (1, 4)))
    out_proj = normal_values(key_list[7], (RET_WIDTH, D), RET_WIDTH ** -0.5, 0.15625, ((0, 4),))
    retained = normal_values(key_list[8], (SEQUENCE_TOKENS, RET_WIDTH), 1.0, 6.0, ((0, 8), (1, 4)))
    queries = normal_values(key_list[9], (SEQUENCE_TOKENS, KEY_WIDTH), 1.0, 6.0, ((0, 8), (1, 4)))
    keys = normal_values(key_list[10], (SEQUENCE_TOKENS, KEY_WIDTH), (KEY_DIM ** -0.5), 0.86328125, ((0, 8), (1, 4)))
    values = normal_values(key_list[11], (SEQUENCE_TOKENS, RET_WIDTH), 1.0, 6.0, ((0, 8), (1, 4)))
    log_decay = draw_log_decay(jax.random.fold_in(key_list[14], 71), 0)
    incoming_state = normal_values(key_list[13], (N_SP, RETENTION_HEADS, KEY_DIM, VALUE_DIM), 1.0, 6.0, ((0, 8), (1, 4)), jnp.float32)
    return dict(moe_input=moe_input, out_grad=out_grad, expert_ids=expert_ids, expert_weights=expert_weights, w_gate=w_gate, w_up=w_up, w_down=w_down, out_proj=out_proj, retained=retained, queries=queries, keys=keys, values=values, log_decay=log_decay, incoming_state=incoming_state)


def slot_table(expert_ids, expert_weights):
    per_block = expert_ids.reshape(N_SP, 2 * TOK_DEV)
    block_weights = expert_weights.reshape(N_SP, 2 * TOK_DEV)
    onehot = (per_block[:, :, None] == jnp.arange(EXPERTS, dtype=jnp.int32)[None, None, :]).astype(jnp.int32)
    ranks = jnp.sum((jnp.cumsum(onehot, axis=1) - onehot) * onehot, axis=2).astype(jnp.int32)
    block = jnp.arange(N_SP, dtype=jnp.int32)[:, None]
    dest = (per_block * (N_SP * CAP) + block * CAP + ranks).reshape(-1).astype(jnp.int32)
    token = (block * TOK_DEV + jnp.arange(2 * TOK_DEV, dtype=jnp.int32)[None, :] // 2).reshape(-1).astype(jnp.int32)
    table = jnp.full((EXPERTS * N_SP * CAP,), SEQUENCE_TOKENS, jnp.int32).at[dest].set(token)
    weight = jnp.zeros((EXPERTS * N_SP * CAP,), jnp.float32).at[dest].set(block_weights.reshape(-1))
    return table.reshape(EXPERTS, N_SP * CAP), weight.reshape(EXPERTS, N_SP * CAP)


def reference(moe_input, out_grad, expert_ids, expert_weights, w_gate, w_up, w_down, out_proj,
              retained, queries, keys, values, log_decay, incoming_state):
    f32 = jnp.float32
    bf16 = jnp.bfloat16
    upper_limit = lax.Precision.HIGHEST
    table, weight = slot_table(expert_ids, expert_weights)
    padded_rows = jnp.concatenate([moe_input, jnp.zeros((1, D), bf16)], axis=0)
    padded_grad = jnp.concatenate([out_grad, jnp.zeros((1, D), bf16)], axis=0)
    part = FF // N_TP

    def expert_back(args):
        index, slot_weight, gate_w, up_w, down_w = args
        rows = padded_rows[index]
        grad = (padded_grad[index].astype(f32) * slot_weight[:, None]).astype(bf16)
        gate = jnp.dot(rows, gate_w, preferred_element_type=f32)
        up = jnp.dot(rows, up_w, preferred_element_type=f32)
        sig = jax.nn.sigmoid(gate)
        swish = gate * sig
        act = (swish * up).astype(bf16)
        act_grad = jnp.dot(grad, down_w.T, preferred_element_type=f32)
        gate_grad = (act_grad * up * sig * (1.0 + gate * (1.0 - sig))).astype(bf16)
        up_grad = (act_grad * swish).astype(bf16)
        down_grad = jnp.dot(act.T, grad, preferred_element_type=f32).astype(bf16)
        gate_w_grad = jnp.dot(rows.T, gate_grad, preferred_element_type=f32).astype(bf16)
        up_w_grad = jnp.dot(rows.T, up_grad, preferred_element_type=f32).astype(bf16)
        slots = rows.shape[0]
        parts = (jnp.einsum('snf,dnf->nsd', gate_grad.astype(f32).reshape(slots, N_TP, part),
                            gate_w.astype(f32).reshape(D, N_TP, part))
                 + jnp.einsum('snf,dnf->nsd', up_grad.astype(f32).reshape(slots, N_TP, part),
                              up_w.astype(f32).reshape(D, N_TP, part)))
        rounded = lax.optimization_barrier(parts.astype(bf16))
        slot_in = jnp.sum(rounded.astype(f32), axis=0).astype(bf16)
        return gate_w_grad, up_w_grad, down_grad, slot_in

    w_gate_grad, w_up_grad, w_down_grad, slot_in = lax.map(expert_back, (table, weight, w_gate, w_up, w_down))
    token_grad = jnp.zeros((SEQUENCE_TOKENS + 1, D), f32).at[table.reshape(-1)].add(
        slot_in.reshape(-1, D).astype(f32))[:SEQUENCE_TOKENS]
    stream = (out_grad.astype(f32) + token_grad).astype(bf16)
    ret_grad = jnp.dot(stream, out_proj.T, preferred_element_type=f32).astype(bf16)
    out_proj_grad = jnp.dot(stream.T, retained, preferred_element_type=f32)

    q = queries.astype(f32).reshape(N_SP, TOK_DEV, RETENTION_HEADS, KEY_DIM)
    k = keys.astype(f32).reshape(N_SP, TOK_DEV, RETENTION_HEADS, KEY_DIM)
    v = values.astype(f32).reshape(N_SP, TOK_DEV, RETENTION_HEADS, VALUE_DIM)
    o = ret_grad.astype(f32).reshape(N_SP, TOK_DEV, RETENTION_HEADS, VALUE_DIM)
    b = jnp.cumsum(log_decay.reshape(N_SP, TOK_DEV, RETENTION_HEADS), axis=1)
    b_end = b[:, -1]
    diff = b[:, :, None, :] - b[:, None, :, :]
    place = jnp.arange(TOK_DEV)
    causal = (place[:, None] >= place[None, :])[None, :, :, None]
    decay = jnp.where(causal, jnp.exp(jnp.minimum(diff, 0.0)), 0.0)
    scores = jnp.einsum('nthk,nshk->ntsh', q, k, precision=upper_limit) * decay
    prob_grad = jnp.einsum('nthv,nshv->ntsh', o, v, precision=upper_limit) * decay
    added_input = jnp.einsum('nth,nthk,nthv->nhkv', jnp.exp(b), q, o, precision=upper_limit)

    def back_step(carry, inputs):
        factor, term = inputs
        return term + factor[:, None, None] * carry, carry

    _, state_gradient = lax.scan(back_step, jnp.zeros((RETENTION_HEADS, KEY_DIM, VALUE_DIM), f32),
                             (jnp.exp(b_end), added_input), reverse=True)
    tail = jnp.exp(b_end[:, None, :] - b)[..., None]
    query_grad = (jnp.einsum('ntsh,nshk->nthk', prob_grad, k, precision=upper_limit)
                  + jnp.exp(b)[..., None] * jnp.einsum('nthv,nhkv->nthk', o, incoming_state, precision=upper_limit))
    key_grad = (jnp.einsum('ntsh,nthk->nshk', prob_grad, q, precision=upper_limit)
                + tail * jnp.einsum('nshv,nhkv->nshk', v, state_gradient, precision=upper_limit))
    value_grad = (jnp.einsum('ntsh,nthv->nshv', scores, o, precision=upper_limit)
                  + tail * jnp.einsum('nshk,nhkv->nshv', k, state_gradient, precision=upper_limit))
    return (w_gate_grad, w_up_grad, w_down_grad, out_proj_grad,
            query_grad.reshape(SEQUENCE_TOKENS, KEY_WIDTH).astype(bf16),
            key_grad.reshape(SEQUENCE_TOKENS, KEY_WIDTH).astype(bf16),
            value_grad.reshape(SEQUENCE_TOKENS, RET_WIDTH).astype(bf16))
```

```python
import functools

import jax
import jax.numpy as jnp
from jax import lax
from jax.experimental import pallas as pl
from jax.experimental.pallas import tpu as pltpu
from jax.sharding import PartitionSpec as P

MESH = pl.DeviceIdType.MESH
F32 = jnp.float32
BF16 = jnp.bfloat16
LIMIT = 60 * 1024 * 1024


def where_am_i(n, ny):
    s, t = lax.axis_index("sp"), lax.axis_index("tp")
    return s, t, lax.div(t, 2), lax.rem(t, 2)


def greet(peers):
    barrier = pltpu.get_barrier_semaphore()
    for peer in peers:
        pl.semaphore_signal(barrier, inc=1, device_id=peer, device_id_type=MESH)
    pl.semaphore_wait(barrier, len(peers))


def sp_peers(n, s, t):
    return [(lax.rem(s + k, n), t) for k in range(1, n)]


def tp_peers(ny, s, y, c):
    return [(s, lax.rem(y + d, ny) * 2 + c) for d in range(1, ny)] + [(s, y * 2 + 1 - c)]


def remote(src, dst, send, recv, peer):
    return pltpu.make_async_remote_copy(
        src_ref=src, dst_ref=dst, send_sem=send, recv_sem=recv, device_id=peer, device_id_type=MESH
    )


def dispatch_kernel(
    n, ny, send_ref, kept_ref, ends_ref, out_ref, kept_out, ends_out,
    local_sem, a_send, a_recv, e_send, e_recv, y_send, y_recv, p_send, p_recv,
    r_send, r_recv, l_send, l_recv, x_send, x_recv,
):
    s, t, y, c = where_am_i(n, ny)
    cap, q = send_ref.shape[2], send_ref.shape[3]
    nz = n // 2
    z, x = lax.div(s, 2), lax.rem(s, 2)
    greet(sp_peers(n, s, t) + tp_peers(ny, s, y, c))
    partner = (s, y * 2 + 1 - c)

    def block(src, tt):
        rows = pl.ds(pl.multiple_of(src * cap, cap), cap)
        columns = pl.ds(pl.multiple_of(tt * q, q), q)
        return out_ref.at[:, rows, columns]

    own = [
        pltpu.make_async_copy(send_ref.at[s], block(s, t), local_sem.at[0]),
        pltpu.make_async_copy(kept_ref, kept_out.at[s], local_sem.at[1]),
        pltpu.make_async_copy(ends_ref, ends_out.at[s], local_sem.at[2]),
    ]
    for copy in own:
        copy.start()
    arrivals, waits = [own[0]], []
    for k in range(1, n):
        peer = lax.rem(s + k, n)
        copy = remote(send_ref.at[peer], block(s, t), a_send.at[k], a_recv.at[k], (peer, t))
        copy.start()
        arrivals.append(copy)
        waits.append(copy.wait_send)
    for k in range(1, n):
        peer = lax.rem(s + k, n)
        copy = remote(ends_ref, ends_out.at[s], e_send.at[k], e_recv.at[k], (peer, t))
        copy.start()
        waits.append(copy.wait)

    def at(zz):
        return lax.rem(zz + 2 * nz, nz) * 2 + x

    def hop(j, sign, send, recv, source):
        held = at(z - sign * j)
        copy = remote(source, kept_out.at[held], send.at[j], recv.at[j], (at(z + sign), t))
        copy.start()
        waits.append(copy.wait_send)
        return copy

    right_steps, left_steps = nz // 2, nz - 1 - nz // 2
    right = hop(0, 1, r_send, r_recv, kept_ref) if right_steps else None
    left = hop(0, -1, l_send, l_recv, kept_ref) if left_steps else None
    pair = (z * 2 + 1 - x, t)

    def across(held, index, source):
        copy = remote(source, kept_out.at[held], x_send.at[index], x_recv.at[index], pair)
        copy.start()
        waits.append(copy.wait)

    across(s, 0, kept_ref)
    from_far = {}
    for k in range(n + 1):
        if k < n:
            src = lax.rem(s - k + n, n)
            if k == 0:
                arrivals[0].wait()
            else:
                arrivals[k].wait_recv()
            mine = block(src, t)
            for d in range(1, ny):
                far = (s, lax.rem(y + d, ny) * 2 + c)
                copy = remote(mine, mine, y_send.at[d, k], y_recv.at[d, k], far)
                copy.start()
                waits.append(copy.wait_send)
                from_far[d, k] = copy
            copy = remote(mine, mine, p_send.at[0, k], p_recv.at[0, k], partner)
            copy.start()
            waits.append(copy.wait)
        if k >= 1:
            src = lax.rem(s - k + 1 + n, n)
            for d in range(1, ny):
                from_far[d, k - 1].wait_recv()
                theirs = block(src, lax.rem(y - d + ny, ny) * 2 + c)
                copy = remote(theirs, theirs, p_send.at[d, k - 1], p_recv.at[d, k - 1], partner)
                copy.start()
                waits.append(copy.wait)
    index = 1
    for j in range(1, right_steps + 1):
        right.wait_recv()
        held = at(z - j)
        if j < right_steps:
            right = hop(j, 1, r_send, r_recv, kept_out.at[held])
        across(held, index, kept_out.at[held])
        index += 1
        if j <= left_steps:
            left.wait_recv()
            held = at(z + j)
            if j < left_steps:
                left = hop(j, -1, l_send, l_recv, kept_out.at[held])
            across(held, index, kept_out.at[held])
            index += 1
    own[1].wait()
    own[2].wait()
    for wait in waits:
        wait()


def dispatch(n, ny, send, kept, ends):
    cap, q = send.shape[2], send.shape[3]
    dma = pltpu.SemaphoreType.DMA
    return pl.pallas_call(
        functools.partial(dispatch_kernel, n, ny),
        out_shape=(
            jax.ShapeDtypeStruct((2, n * cap, q * ny * 2), BF16),
            jax.ShapeDtypeStruct((n,) + kept.shape, BF16),
            jax.ShapeDtypeStruct((n,) + ends.shape, F32),
        ),
        in_specs=[pl.BlockSpec(memory_space=pltpu.VMEM)] * 3,
        out_specs=[pl.BlockSpec(memory_space=pltpu.VMEM)] * 3,
        scratch_shapes=[dma((3,)), dma((n,)), dma((n,)), dma((n,)), dma((n,))]
        + [dma((ny, n))] * 4
        + [dma((n,))] * 6,
        compiler_params=pltpu.CompilerParams(
            collective_id=0, has_side_effects=True, vmem_limit_bytes=LIMIT
        ),
    )(send, kept, ends)


def combine_kernel(
    n, ny, part_ref, pick_ref, grad_ref, stream_ref, near, pairs, far, share, back,
    p_send, p_recv, y_send, y_recv, a_send, a_recv, g_send, g_recv, h_send, h_recv,
):
    s, t, y, c = where_am_i(n, ny)
    q = grad_ref.shape[1]
    cap = part_ref.shape[0] // n
    greet(sp_peers(n, s, t) + tp_peers(ny, s, y, c))
    partner = (s, y * 2 + 1 - c)
    waits = []

    def columns(tt):
        return pl.ds(pl.multiple_of(tt * q, q), q)

    def rows(b):
        return pl.ds(pl.multiple_of(b * cap, cap), cap)

    halves = {}
    for d in list(range(1, ny)) + [0]:
        theirs = lax.rem(y + d, ny) * 2 + 1 - c
        copy = remote(
            part_ref.at[:, columns(theirs)], near.at[d], p_send.at[d], p_recv.at[d], partner
        )
        copy.start()
        waits.append(copy.wait_send)
        halves[d] = copy
    arrived = {}
    for d in range(1, ny):
        halves[d].wait_recv()
        tt = lax.rem(y + d, ny) * 2 + c
        for k in range(1, n + 1):
            b = rows(lax.rem(s + k, n))
            pairs[d, b, :] = (
                part_ref[b, columns(tt)].astype(F32) + near[d, b, :].astype(F32)
            ).astype(BF16)
        for k in range(1, n + 1):
            b = rows(lax.rem(s + k, n))
            copy = remote(
                pairs.at[d, b, :], far.at[d, b, :],
                y_send.at[d, k % n], y_recv.at[d, k % n], (s, tt),
            )
            copy.start()
            waits.append(copy.wait_send)
            arrived[d, k] = copy
    halves[0].wait_recv()
    returns = []
    for k in range(1, n + 1):
        peer = lax.rem(s + k, n)
        b = rows(peer)
        total = part_ref[b, columns(t)].astype(F32) + near[0, b, :].astype(F32)
        for d in range(1, ny):
            arrived[d, k].wait_recv()
            total = total + far[d, b, :].astype(F32)
        if k < n:
            share[b, :] = total.astype(BF16)
            copy = remote(
                share.at[b, :], back.at[rows(s), :], a_send.at[k], a_recv.at[k], (peer, t)
            )
            copy.start()
            waits.append(copy.wait_send)
            returns.append(copy)
        else:
            back[b, :] = total.astype(BF16)
    for copy in returns:
        copy.wait_recv()
    token = jnp.dot(pick_ref[...], back[...], preferred_element_type=F32)
    stream_ref[:, columns(t)] = (grad_ref[...].astype(F32) + token).astype(BF16)
    mine = stream_ref.at[:, columns(t)]
    outer = []
    for d in range(1, ny):
        copy = remote(
            mine, mine, g_send.at[d], g_recv.at[d], (s, lax.rem(y + d, ny) * 2 + c)
        )
        copy.start()
        waits.append(copy.wait_send)
        outer.append(copy)
    copy = remote(mine, mine, h_send.at[0], h_recv.at[0], partner)
    copy.start()
    waits.append(copy.wait)
    for d in range(1, ny):
        outer[d - 1].wait_recv()
        theirs = stream_ref.at[:, columns(lax.rem(y - d + ny, ny) * 2 + c)]
        copy = remote(theirs, theirs, h_send.at[d], h_recv.at[d], partner)
        copy.start()
        waits.append(copy.wait)
    for wait in waits:
        wait()


def combine(n, ny, part, pick, grad):
    slots, q = part.shape[0], grad.shape[1]
    dma = pltpu.SemaphoreType.DMA
    return pl.pallas_call(
        functools.partial(combine_kernel, n, ny),
        out_shape=jax.ShapeDtypeStruct((grad.shape[0], q * ny * 2), BF16),
        in_specs=[pl.BlockSpec(memory_space=pltpu.VMEM)] * 3,
        out_specs=pl.BlockSpec(memory_space=pltpu.VMEM),
        scratch_shapes=[pltpu.VMEM((ny, slots, q), BF16)] * 3
        + [pltpu.VMEM((slots, q), BF16)] * 2
        + [dma((ny,))] * 2
        + [dma((ny, n))] * 2
        + [dma((n,))] * 2
        + [dma((ny,))] * 4,
        compiler_params=pltpu.CompilerParams(
            collective_id=1, has_side_effects=True, vmem_limit_bytes=LIMIT
        ),
    )(part, pick, grad)


def tail_kernel(
    n, ny, stream_ref, state_ref, cols_ref, states_ref,
    local_sem, a_send, a_recv, i_send, i_recv, p_send, p_recv,
):
    s, t, y, c = where_am_i(n, ny)
    half = stream_ref.shape[1] // 2
    partner = (s, y * 2 + 1 - c)
    greet(sp_peers(n, s, t) + [partner])
    band = pl.ds(pl.multiple_of(c * half, half), half)
    own = [
        pltpu.make_async_copy(stream_ref.at[s], cols_ref.at[s], local_sem.at[0]),
        pltpu.make_async_copy(state_ref, states_ref.at[s], local_sem.at[1]),
    ]
    for copy in own:
        copy.start()
    waits, arrivals = [copy.wait for copy in own], []
    for k in range(1, n):
        peer = lax.rem(s + k, n)
        copy = remote(state_ref, states_ref.at[s], i_send.at[k], i_recv.at[k], (peer, t))
        copy.start()
        waits.append(copy.wait)
    for k in range(1, n):
        peer = lax.rem(s + k, n)
        copy = remote(
            stream_ref.at[peer, band], cols_ref.at[s, band], a_send.at[k], a_recv.at[k], (peer, t)
        )
        copy.start()
        waits.append(copy.wait_send)
        arrivals.append(copy)
    for k in range(1, n):
        arrivals[k - 1].wait_recv()
        held = cols_ref.at[lax.rem(s - k + n, n), band]
        copy = remote(held, held, p_send.at[k], p_recv.at[k], partner)
        copy.start()
        waits.append(copy.wait)
    for wait in waits:
        wait()


def tail_exchange(n, ny, stream, state):
    dma = pltpu.SemaphoreType.DMA
    return pl.pallas_call(
        functools.partial(tail_kernel, n, ny),
        out_shape=(
            jax.ShapeDtypeStruct(stream.shape, BF16),
            jax.ShapeDtypeStruct((n,) + state.shape, state.dtype),
        ),
        in_specs=[pl.BlockSpec(memory_space=pltpu.VMEM)] * 2,
        out_specs=[pl.BlockSpec(memory_space=pltpu.VMEM)] * 2,
        scratch_shapes=[dma((2,))] + [dma((n,))] * 6,
        compiler_params=pltpu.CompilerParams(
            collective_id=2, has_side_effects=True, vmem_limit_bytes=LIMIT
        ),
    )(stream, state)


def expert_back(rows, grad, gate_w, up_w, down_w):
    f32 = jnp.float32
    bf16 = jnp.bfloat16
    gate = jnp.dot(rows, gate_w, preferred_element_type=f32)
    up = jnp.dot(rows, up_w, preferred_element_type=f32)
    sig = jax.nn.sigmoid(gate)
    swish = gate * sig
    act = (swish * up).astype(bf16)
    across = (((1,), (1,)), ((), ()))
    along = (((0,), (0,)), ((), ()))
    act_grad = lax.dot_general(grad, down_w, across, preferred_element_type=f32)
    gate_grad = (act_grad * up * sig * (1.0 + gate * (1.0 - sig))).astype(bf16)
    up_grad = (act_grad * swish).astype(bf16)
    down_grad = lax.dot_general(act, grad, along, preferred_element_type=f32).astype(bf16)
    gate_w_grad = lax.dot_general(rows, gate_grad, along, preferred_element_type=f32).astype(bf16)
    up_w_grad = lax.dot_general(rows, up_grad, along, preferred_element_type=f32).astype(bf16)
    partial_value = lax.dot_general(
        gate_grad, gate_w, across, preferred_element_type=f32
    ) + lax.dot_general(up_grad, up_w, across, preferred_element_type=f32)
    return (gate_w_grad, up_w_grad, down_grad, partial_value)


def on_device(
    moe_input,
    out_grad,
    expert_ids,
    expert_weights,
    w_gate,
    w_up,
    w_down,
    out_proj,
    retained,
    queries,
    keys,
    values,
    log_decay,
    incoming_state,
):
    f32 = jnp.float32
    bf16 = jnp.bfloat16
    upper_limit = lax.Precision.HIGHEST
    tokens_here = moe_input.shape[0]
    width = moe_input.shape[1]
    sp_count = lax.axis_size("sp")
    tp_count = lax.axis_size("tp")
    capacity = -(-(5 * tokens_here // (2 * sp_count)) // 16) * 16
    slot_count = sp_count * capacity
    flat_ids = expert_ids.reshape(-1)
    flat_weights = expert_weights.reshape(-1)
    onehot = (flat_ids[:, None] == jnp.arange(sp_count, dtype=jnp.int32)[None, :]).astype(jnp.int32)
    ranks = jnp.sum((jnp.cumsum(onehot, axis=0) - onehot) * onehot, axis=1)
    slot_of = flat_ids * capacity + ranks
    hits = jnp.arange(slot_count, dtype=jnp.int32)[:, None] == slot_of[None, :]
    picker = jnp.any(hits.reshape(slot_count, tokens_here, 2), axis=2).astype(bf16)
    slot_weight = jnp.sum(jnp.where(hits, flat_weights[None, :], 0.0), axis=1)
    along = (((0,), (0,)), ((), ()))
    column_count = width // tp_count
    ny = tp_count // 2
    heads_here = log_decay.shape[1]
    running_total = jnp.cumsum(log_decay, axis=0)
    last_sum = running_total[-1]
    own_rows = lax.dynamic_slice_in_dim(
        moe_input, lax.axis_index("tp") * column_count, column_count, 1
    )
    send_rows = jnp.dot(picker, own_rows, preferred_element_type=f32).astype(bf16)
    send_grad = (
        jnp.dot(picker, out_grad, preferred_element_type=f32) * slot_weight[:, None]
    ).astype(bf16)
    send = jnp.stack(
        [part.reshape(sp_count, capacity, column_count) for part in (send_rows, send_grad)], axis=1
    )
    ends = jnp.zeros((8, 128), f32).at[:, :heads_here].set(last_sum[None, :])
    received, kept_all, ends_all = dispatch(sp_count, ny, send, retained, ends)
    gate_w_grad, up_w_grad, down_grad, partial_value = expert_back(
        received[0], received[1], w_gate[0], w_up[0], w_down[0]
    )
    stream = combine(sp_count, ny, partial_value.astype(bf16), picker.T, out_grad)
    ret_grad = lax.dot_general(
        stream, out_proj, (((1,), (1,)), ((), ())), preferred_element_type=f32
    ).astype(bf16)
    key_dim = queries.shape[1] // heads_here
    value_dim = values.shape[1] // heads_here
    query_rows = queries.astype(f32).reshape(tokens_here, heads_here, key_dim)
    key_matrix = keys.astype(f32).reshape(tokens_here, heads_here, key_dim)
    value_matrix = values.astype(f32).reshape(tokens_here, heads_here, value_dim)
    incoming_gradient = ret_grad.astype(f32).reshape(tokens_here, heads_here, value_dim)
    place = jnp.arange(tokens_here)
    causal = (place[:, None] >= place[None, :])[:, :, None]
    diff = running_total[:, None, :] - running_total[None, :, :]
    decay = jnp.where(causal, jnp.exp(jnp.minimum(diff, 0.0)), 0.0)
    scores = jnp.einsum("thk,shk->tsh", query_rows, key_matrix, precision=upper_limit) * decay
    prob_grad = (
        jnp.einsum("thv,shv->tsh", incoming_gradient, value_matrix, precision=upper_limit) * decay
    )
    added_input = jnp.einsum(
        "yb,ybm,ybx->bmx",
        jnp.exp(running_total),
        query_rows,
        incoming_gradient,
        precision=upper_limit,
    )
    flat_state = added_input.transpose(1, 0, 2).reshape(key_dim, heads_here * value_dim)
    stream_blocks = stream.reshape(tokens_here, sp_count, width // sp_count).transpose(1, 0, 2)
    stream_all, states = tail_exchange(sp_count, ny, stream_blocks, flat_state.astype(bf16))
    out_proj_grad = lax.dot_general(
        stream_all.reshape(sp_count * tokens_here, -1),
        kept_all.reshape(sp_count * tokens_here, -1),
        along,
        preferred_element_type=f32,
    )
    block_ends = ends_all[:, 0, :heads_here]
    before = jnp.cumsum(block_ends, axis=0) - block_ends
    here = lax.axis_index("sp")
    since = jnp.sum(
        jnp.where(jnp.arange(sp_count)[:, None] <= here, block_ends, 0.0), axis=0, keepdims=True
    )
    reach = jnp.where(
        jnp.arange(sp_count)[:, None] > here, jnp.exp(jnp.minimum(before - since, 0.0)), 0.0
    )
    state_gradient = jnp.sum(
        states.astype(f32).reshape(sp_count, key_dim, heads_here, value_dim)
        * reach[:, None, :, None],
        axis=0,
    ).transpose(1, 0, 2)
    tail = jnp.exp(last_sum[None, :] - running_total)[..., None]
    query_grad = jnp.einsum("tsh,shk->thk", prob_grad, key_matrix, precision=upper_limit) + jnp.exp(
        running_total
    )[..., None] * jnp.einsum(
        "ybc,bfc->ybf", incoming_gradient, incoming_state[0], precision=upper_limit
    )
    key_grad = jnp.einsum(
        "tsh,thk->shk", prob_grad, query_rows, precision=upper_limit
    ) + tail * jnp.einsum("rgd,gnd->rgn", value_matrix, state_gradient, precision=upper_limit)
    value_grad = jnp.einsum(
        "tsh,thv->shv", scores, incoming_gradient, precision=upper_limit
    ) + tail * jnp.einsum("bgi,gie->bge", key_matrix, state_gradient, precision=upper_limit)
    return (
        gate_w_grad[None],
        up_w_grad[None],
        down_grad[None],
        out_proj_grad,
        query_grad.reshape(tokens_here, -1).astype(bf16),
        key_grad.reshape(tokens_here, -1).astype(bf16),
        value_grad.reshape(tokens_here, -1).astype(bf16),
    )


def solution(mesh):
    placed = (
        P("sp", None),
        P("sp", "tp"),
        P("sp", None),
        P("sp", None),
        P("sp", None, "tp"),
        P("sp", None, "tp"),
        P("sp", "tp", None),
        P("tp", None),
        P("sp", "tp"),
        P("sp", "tp"),
        P("sp", "tp"),
        P("sp", "tp"),
        P("sp", "tp"),
        P("sp", "tp", None, None),
    )
    return jax.shard_map(
        on_device,
        mesh=mesh,
        in_specs=placed,
        out_specs=(
            P("sp", None, "tp"),
            P("sp", None, "tp"),
            P("sp", "tp", None),
            P("sp", "tp"),
            P("sp", "tp"),
            P("sp", "tp"),
            P("sp", "tp"),
        ),
        check_vma=False,
    )
```

```python
import functools

import jax
import jax.numpy as jnp
from jax import lax
from jax.experimental import pallas as pl
from jax.experimental.pallas import tpu as pltpu
from jax.sharding import PartitionSpec as P

MESH = pl.DeviceIdType.MESH
F32 = jnp.float32
BF16 = jnp.bfloat16
LIMIT = 60 * 1024 * 1024


def where_am_i(n, ny):
    s, t = lax.axis_index("sp"), lax.axis_index("tp")
    return s, t, lax.div(t, 2), lax.rem(t, 2)


def greet(peers):
    barrier = pltpu.get_barrier_semaphore()
    for peer in peers:
        pl.semaphore_signal(barrier, inc=1, device_id=peer, device_id_type=MESH)
    pl.semaphore_wait(barrier, len(peers))


def sp_peers(n, s, t):
    return [(lax.rem(s + k, n), t) for k in range(1, n)]


def tp_peers(ny, s, y, c):
    return [(s, lax.rem(y + d, ny) * 2 + c) for d in range(1, ny)] + [(s, y * 2 + 1 - c)]


def remote(src, dst, send, recv, peer):
    return pltpu.make_async_remote_copy(
        src_ref=src, dst_ref=dst, send_sem=send, recv_sem=recv, device_id=peer, device_id_type=MESH
    )


def dispatch_kernel(
    n, ny, cap, route_ref, decay_ref, rows_ref, grad_ref, out_ref, pick_ref, ends_out,
    send_ref, local_sem, a_send, a_recv, e_send, e_recv, y_send, y_recv, p_send, p_recv,
):
    s, t, y, c = where_am_i(n, ny)
    q = grad_ref.shape[1]
    tokens, heads = decay_ref.shape
    partner = (s, y * 2 + 1 - c)

    ids = [route_ref[j : j + 1, :] for j in range(2)]
    weights = [route_ref[j : j + 1, :] for j in range(2, 4)]
    expert = lax.broadcasted_iota(jnp.int32, (n, tokens), 0).astype(F32)
    named = [(expert == own).astype(F32) for own in ids]
    first = lax.broadcasted_iota(jnp.int32, (tokens, tokens), 0)
    second = lax.broadcasted_iota(jnp.int32, (tokens, tokens), 1)
    earlier = jnp.dot(
        (named[0] + named[1]).astype(BF16),
        (first < second).astype(F32).astype(BF16),
        preferred_element_type=F32,
    )
    slot = [
        own * cap + jnp.sum(hot * earlier, axis=0, keepdims=True) for own, hot in zip(ids, named)
    ]
    number = lax.broadcasted_iota(jnp.int32, (n * cap, tokens), 0).astype(F32)
    hits = [(number == own).astype(F32) for own in slot]
    picker = (hits[0] + hits[1]).astype(BF16)
    slot_weight = jnp.sum(hits[0] * weights[0] + hits[1] * weights[1], axis=1, keepdims=True)
    pick_ref[...] = picker
    ends_out[s, :, :] = jnp.zeros((8, 128), F32)
    ends_out[s, :, pl.ds(0, heads)] = jnp.broadcast_to(
        jnp.sum(decay_ref[...], axis=0, keepdims=True), (8, heads)
    )
    own_rows = rows_ref[:, pl.ds(pl.multiple_of(t * q, q), q)]
    picked = jnp.dot(picker, own_rows, preferred_element_type=F32).astype(BF16)
    send_ref[:, 0] = picked.reshape(n, cap, q)
    cotangent = jnp.dot(picker, grad_ref[...], preferred_element_type=F32) * slot_weight
    send_ref[:, 1] = cotangent.astype(BF16).reshape(n, cap, q)

    greet(sp_peers(n, s, t) + tp_peers(ny, s, y, c))

    def block(src, tt):
        rows = pl.ds(pl.multiple_of(src * cap, cap), cap)
        columns = pl.ds(pl.multiple_of(tt * q, q), q)
        return out_ref.at[:, rows, columns]

    own = pltpu.make_async_copy(send_ref.at[s], block(s, t), local_sem.at[0])
    own.start()
    arrivals, waits = [own], []
    for k in range(1, n):
        peer = lax.rem(s + k, n)
        copy = remote(send_ref.at[peer], block(s, t), a_send.at[k], a_recv.at[k], (peer, t))
        copy.start()
        arrivals.append(copy)
        waits.append(copy.wait_send)
    for k in range(1, n):
        peer = lax.rem(s + k, n)
        copy = remote(ends_out.at[s], ends_out.at[s], e_send.at[k], e_recv.at[k], (peer, t))
        copy.start()
        waits.append(copy.wait)
    from_far = {}
    for k in range(n + 1):
        if k < n:
            src = lax.rem(s - k + n, n)
            if k == 0:
                arrivals[0].wait()
            else:
                arrivals[k].wait_recv()
            mine = block(src, t)
            for d in range(1, ny):
                far = (s, lax.rem(y + d, ny) * 2 + c)
                copy = remote(mine, mine, y_send.at[d, k], y_recv.at[d, k], far)
                copy.start()
                waits.append(copy.wait_send)
                from_far[d, k] = copy
            copy = remote(mine, mine, p_send.at[0, k], p_recv.at[0, k], partner)
            copy.start()
            waits.append(copy.wait)
        if k >= 1:
            src = lax.rem(s - k + 1 + n, n)
            for d in range(1, ny):
                from_far[d, k - 1].wait_recv()
                theirs = block(src, lax.rem(y - d + ny, ny) * 2 + c)
                copy = remote(theirs, theirs, p_send.at[d, k - 1], p_recv.at[d, k - 1], partner)
                copy.start()
                waits.append(copy.wait)
    for wait in waits:
        wait()


def dispatch(n, ny, cap, route, decay, rows, grad):
    tokens, q = grad.shape
    dma = pltpu.SemaphoreType.DMA
    return pl.pallas_call(
        functools.partial(dispatch_kernel, n, ny, cap),
        out_shape=(
            jax.ShapeDtypeStruct((2, n * cap, q * ny * 2), BF16),
            jax.ShapeDtypeStruct((n * cap, tokens), BF16),
            jax.ShapeDtypeStruct((n, 8, 128), F32),
        ),
        in_specs=[pl.BlockSpec(memory_space=pltpu.VMEM)] * 4,
        out_specs=[pl.BlockSpec(memory_space=pltpu.VMEM)] * 3,
        scratch_shapes=[pltpu.VMEM((n, 2, cap, q), BF16)]
        + [dma((1,)), dma((n,)), dma((n,)), dma((n,)), dma((n,))]
        + [dma((ny, n))] * 4,
        compiler_params=pltpu.CompilerParams(
            collective_id=0, has_side_effects=True, vmem_limit_bytes=LIMIT
        ),
    )(route, decay, rows, grad)


def combine_kernel(
    n, ny, part_ref, pick_ref, grad_ref, kept_ref, stream_ref, blocks_ref, kept_out,
    near, pairs, far, share, back,
    p_send, p_recv, y_send, y_recv, a_send, a_recv, g_send, g_recv, h_send, h_recv,
    local_sem, r_send, r_recv, l_send, l_recv, x_send, x_recv,
):
    s, t, y, c = where_am_i(n, ny)
    q = grad_ref.shape[1]
    cap = part_ref.shape[0] // n
    greet(sp_peers(n, s, t) + tp_peers(ny, s, y, c))
    partner = (s, y * 2 + 1 - c)
    waits = []

    def columns(tt):
        return pl.ds(pl.multiple_of(tt * q, q), q)

    def rows(b):
        return pl.ds(pl.multiple_of(b * cap, cap), cap)

    nz = n // 2
    z, x = lax.div(s, 2), lax.rem(s, 2)
    pair = (z * 2 + 1 - x, t)
    kept_own = pltpu.make_async_copy(kept_ref, kept_out.at[s], local_sem.at[0])
    kept_own.start()
    waits.append(kept_own.wait)

    def at(zz):
        return lax.rem(zz + 2 * nz, nz) * 2 + x

    def hop(j, sign, send, recv, source):
        held = at(z - sign * j)
        copy = remote(source, kept_out.at[held], send.at[j], recv.at[j], (at(z + sign), t))
        copy.start()
        waits.append(copy.wait_send)
        return copy

    def across(held, index, source):
        copy = remote(source, kept_out.at[held], x_send.at[index], x_recv.at[index], pair)
        copy.start()
        waits.append(copy.wait)

    right_steps, left_steps = nz // 2, nz - 1 - nz // 2
    moving = {}

    def relay(j):
        if j <= right_steps:
            moving["right"].wait_recv()
            held = at(z - j)
            if j < right_steps:
                moving["right"] = hop(j, 1, r_send, r_recv, kept_out.at[held])
            across(held, 2 * j - 1, kept_out.at[held])
        if j <= left_steps:
            moving["left"].wait_recv()
            held = at(z + j)
            if j < left_steps:
                moving["left"] = hop(j, -1, l_send, l_recv, kept_out.at[held])
            across(held, 2 * j, kept_out.at[held])

    halves = {}
    for d in list(range(1, ny)) + [0]:
        theirs = lax.rem(y + d, ny) * 2 + 1 - c
        copy = remote(
            part_ref.at[:, columns(theirs)], near.at[d], p_send.at[d], p_recv.at[d], partner
        )
        copy.start()
        waits.append(copy.wait_send)
        halves[d] = copy
    if right_steps:
        moving["right"] = hop(0, 1, r_send, r_recv, kept_ref)
    if left_steps:
        moving["left"] = hop(0, -1, l_send, l_recv, kept_ref)
    across(s, 0, kept_ref)
    arrived = {}
    for d in range(1, ny):
        halves[d].wait_recv()
        tt = lax.rem(y + d, ny) * 2 + c
        for k in range(1, n + 1):
            b = rows(lax.rem(s + k, n))
            pairs[d, b, :] = (
                part_ref[b, columns(tt)].astype(F32) + near[d, b, :].astype(F32)
            ).astype(BF16)
        for k in range(1, n + 1):
            b = rows(lax.rem(s + k, n))
            copy = remote(
                pairs.at[d, b, :], far.at[d, b, :],
                y_send.at[d, k % n], y_recv.at[d, k % n], (s, tt),
            )
            copy.start()
            waits.append(copy.wait_send)
            arrived[d, k] = copy
    halves[0].wait_recv()
    returns = []
    for k in range(1, n + 1):
        peer = lax.rem(s + k, n)
        b = rows(peer)
        total = part_ref[b, columns(t)].astype(F32) + near[0, b, :].astype(F32)
        for d in range(1, ny):
            arrived[d, k].wait_recv()
            total = total + far[d, b, :].astype(F32)
        if k < n:
            share[b, :] = total.astype(BF16)
            copy = remote(
                share.at[b, :], back.at[rows(s), :], a_send.at[k], a_recv.at[k], (peer, t)
            )
            copy.start()
            waits.append(copy.wait_send)
            returns.append(copy)
        else:
            back[b, :] = total.astype(BF16)
        if k % 2 == 0:
            relay(k // 2)
    for copy in returns:
        copy.wait_recv()
    token = lax.dot_general(
        pick_ref[...], back[...], (((0,), (0,)), ((), ())), preferred_element_type=F32
    )
    stream_ref[:, columns(t)] = (grad_ref[...].astype(F32) + token).astype(BF16)
    mine = stream_ref.at[:, columns(t)]
    outer = []
    for d in range(1, ny):
        copy = remote(
            mine, mine, g_send.at[d], g_recv.at[d], (s, lax.rem(y + d, ny) * 2 + c)
        )
        copy.start()
        waits.append(copy.wait_send)
        outer.append(copy)
    copy = remote(mine, mine, h_send.at[0], h_recv.at[0], partner)
    copy.start()
    waits.append(copy.wait)
    for d in range(1, ny):
        outer[d - 1].wait_recv()
        theirs = stream_ref.at[:, columns(lax.rem(y - d + ny, ny) * 2 + c)]
        copy = remote(theirs, theirs, h_send.at[d], h_recv.at[d], partner)
        copy.start()
        waits.append(copy.wait)
    for wait in waits:
        wait()
    wide = blocks_ref.shape[2]
    for b in range(n):
        blocks_ref[b] = stream_ref[:, b * wide : (b + 1) * wide]


def combine(n, ny, part, pick, grad, kept):
    slots, q = part.shape[0], grad.shape[1]
    dma = pltpu.SemaphoreType.DMA
    return pl.pallas_call(
        functools.partial(combine_kernel, n, ny),
        out_shape=(
            jax.ShapeDtypeStruct((grad.shape[0], q * ny * 2), BF16),
            jax.ShapeDtypeStruct((n, grad.shape[0], q * ny * 2 // n), BF16),
            jax.ShapeDtypeStruct((n,) + kept.shape, BF16),
        ),
        in_specs=[pl.BlockSpec(memory_space=pltpu.VMEM)] * 4,
        out_specs=[pl.BlockSpec(memory_space=pltpu.VMEM)] * 3,
        scratch_shapes=[pltpu.VMEM((ny, slots, q), BF16)] * 3
        + [pltpu.VMEM((slots, q), BF16)] * 2
        + [dma((ny,))] * 2
        + [dma((ny, n))] * 2
        + [dma((n,))] * 2
        + [dma((ny,))] * 4
        + [dma((1,))]
        + [dma((n,))] * 6,
        compiler_params=pltpu.CompilerParams(
            collective_id=1, has_side_effects=True, vmem_limit_bytes=LIMIT
        ),
    )(part, pick, grad, kept)


def tail_kernel(
    n, ny, stream_ref, state_ref, cols_ref, states_ref,
    local_sem, a_send, a_recv, i_send, i_recv, p_send, p_recv,
):
    s, t, y, c = where_am_i(n, ny)
    half = stream_ref.shape[1] // 2
    partner = (s, y * 2 + 1 - c)
    greet(sp_peers(n, s, t) + [partner])
    band = pl.ds(pl.multiple_of(c * half, half), half)
    own = [
        pltpu.make_async_copy(stream_ref.at[s], cols_ref.at[s], local_sem.at[0]),
        pltpu.make_async_copy(state_ref, states_ref.at[s], local_sem.at[1]),
    ]
    for copy in own:
        copy.start()
    waits, arrivals = [copy.wait for copy in own], []
    for k in range(1, n):
        peer = lax.rem(s + k, n)
        copy = remote(state_ref, states_ref.at[s], i_send.at[k], i_recv.at[k], (peer, t))
        copy.start()
        waits.append(copy.wait)
    for k in range(1, n):
        peer = lax.rem(s + k, n)
        copy = remote(
            stream_ref.at[peer, band], cols_ref.at[s, band], a_send.at[k], a_recv.at[k], (peer, t)
        )
        copy.start()
        waits.append(copy.wait_send)
        arrivals.append(copy)
    for k in range(1, n):
        arrivals[k - 1].wait_recv()
        held = cols_ref.at[lax.rem(s - k + n, n), band]
        copy = remote(held, held, p_send.at[k], p_recv.at[k], partner)
        copy.start()
        waits.append(copy.wait)
    for wait in waits:
        wait()


def tail_exchange(n, ny, stream, state):
    dma = pltpu.SemaphoreType.DMA
    return pl.pallas_call(
        functools.partial(tail_kernel, n, ny),
        out_shape=(
            jax.ShapeDtypeStruct(stream.shape, BF16),
            jax.ShapeDtypeStruct((n,) + state.shape, state.dtype),
        ),
        in_specs=[pl.BlockSpec(memory_space=pltpu.VMEM)] * 2,
        out_specs=[pl.BlockSpec(memory_space=pltpu.VMEM)] * 2,
        scratch_shapes=[dma((2,))] + [dma((n,))] * 6,
        compiler_params=pltpu.CompilerParams(
            collective_id=2, has_side_effects=True, vmem_limit_bytes=LIMIT
        ),
    )(stream, state)


def expert_back(rows, grad, gate_w, up_w, down_w):
    f32 = jnp.float32
    bf16 = jnp.bfloat16
    gate = jnp.dot(rows, gate_w, preferred_element_type=f32)
    up = jnp.dot(rows, up_w, preferred_element_type=f32)
    sig = jax.nn.sigmoid(gate)
    swish = gate * sig
    act = (swish * up).astype(bf16)
    across = (((1,), (1,)), ((), ()))
    along = (((0,), (0,)), ((), ()))
    act_grad = lax.dot_general(grad, down_w, across, preferred_element_type=f32)
    gate_grad = (act_grad * up * sig * (1.0 + gate * (1.0 - sig))).astype(bf16)
    up_grad = (act_grad * swish).astype(bf16)
    down_grad = lax.dot_general(act, grad, along, preferred_element_type=f32).astype(bf16)
    gate_w_grad = lax.dot_general(rows, gate_grad, along, preferred_element_type=f32).astype(bf16)
    up_w_grad = lax.dot_general(rows, up_grad, along, preferred_element_type=f32).astype(bf16)
    partial_value = lax.dot_general(
        gate_grad, gate_w, across, preferred_element_type=f32
    ) + lax.dot_general(up_grad, up_w, across, preferred_element_type=f32)
    return (gate_w_grad, up_w_grad, down_grad, partial_value)


def on_device(
    moe_input,
    out_grad,
    expert_ids,
    expert_weights,
    w_gate,
    w_up,
    w_down,
    out_proj,
    retained,
    queries,
    keys,
    values,
    log_decay,
    incoming_state,
):
    f32 = jnp.float32
    bf16 = jnp.bfloat16
    upper_limit = lax.Precision.HIGHEST
    tokens_here = moe_input.shape[0]
    sp_count = lax.axis_size("sp")
    tp_count = lax.axis_size("tp")
    capacity = -(-(5 * tokens_here // (2 * sp_count)) // 16) * 16
    along = (((0,), (0,)), ((), ()))
    ny = tp_count // 2
    heads_here = log_decay.shape[1]
    running_total = jnp.cumsum(log_decay, axis=0)
    last_sum = running_total[-1]
    route = jnp.concatenate([expert_ids.astype(f32).T, expert_weights.T], axis=0)
    received, picker, ends_all = dispatch(
        sp_count, ny, capacity, route, log_decay, moe_input, out_grad
    )
    gate_w_grad, up_w_grad, down_grad, partial_value = expert_back(
        received[0], received[1], w_gate[0], w_up[0], w_down[0]
    )
    stream, stream_blocks, kept_all = combine(
        sp_count, ny, partial_value.astype(bf16), picker, out_grad, retained
    )
    ret_grad = lax.dot_general(
        stream, out_proj, (((1,), (1,)), ((), ())), preferred_element_type=f32
    ).astype(bf16)
    key_dim = queries.shape[1] // heads_here
    value_dim = values.shape[1] // heads_here
    query_rows = queries.astype(f32).reshape(tokens_here, heads_here, key_dim)
    key_matrix = keys.astype(f32).reshape(tokens_here, heads_here, key_dim)
    value_matrix = values.astype(f32).reshape(tokens_here, heads_here, value_dim)
    incoming_gradient = ret_grad.astype(f32).reshape(tokens_here, heads_here, value_dim)
    place = jnp.arange(tokens_here)
    causal = (place[:, None] >= place[None, :])[:, :, None]
    diff = running_total[:, None, :] - running_total[None, :, :]
    decay = jnp.where(causal, jnp.exp(jnp.minimum(diff, 0.0)), 0.0)
    scores = jnp.einsum("thk,shk->tsh", query_rows, key_matrix, precision=upper_limit) * decay
    prob_grad = (
        jnp.einsum("thv,shv->tsh", incoming_gradient, value_matrix, precision=upper_limit) * decay
    )
    added_input = jnp.einsum(
        "yb,ybm,ybx->bmx",
        jnp.exp(running_total),
        query_rows,
        incoming_gradient,
        precision=upper_limit,
    )
    flat_state = added_input.transpose(1, 0, 2).reshape(key_dim, heads_here * value_dim)
    stream_all, states = tail_exchange(sp_count, ny, stream_blocks, flat_state.astype(bf16))
    out_proj_grad = lax.dot_general(
        stream_all.reshape(sp_count * tokens_here, -1),
        kept_all.reshape(sp_count * tokens_here, -1),
        along,
        preferred_element_type=f32,
    )
    block_ends = ends_all[:, 0, :heads_here]
    before = jnp.cumsum(block_ends, axis=0) - block_ends
    here = lax.axis_index("sp")
    since = jnp.sum(
        jnp.where(jnp.arange(sp_count)[:, None] <= here, block_ends, 0.0), axis=0, keepdims=True
    )
    reach = jnp.where(
        jnp.arange(sp_count)[:, None] > here, jnp.exp(jnp.minimum(before - since, 0.0)), 0.0
    )
    state_gradient = jnp.sum(
        states.astype(f32).reshape(sp_count, key_dim, heads_here, value_dim)
        * reach[:, None, :, None],
        axis=0,
    ).transpose(1, 0, 2)
    tail = jnp.exp(last_sum[None, :] - running_total)[..., None]
    query_grad = jnp.einsum("tsh,shk->thk", prob_grad, key_matrix, precision=upper_limit) + jnp.exp(
        running_total
    )[..., None] * jnp.einsum(
        "ybc,bfc->ybf", incoming_gradient, incoming_state[0], precision=upper_limit
    )
    key_grad = jnp.einsum(
        "tsh,thk->shk", prob_grad, query_rows, precision=upper_limit
    ) + tail * jnp.einsum("rgd,gnd->rgn", value_matrix, state_gradient, precision=upper_limit)
    value_grad = jnp.einsum(
        "tsh,thv->shv", scores, incoming_gradient, precision=upper_limit
    ) + tail * jnp.einsum("bgi,gie->bge", key_matrix, state_gradient, precision=upper_limit)
    return (
        gate_w_grad[None],
        up_w_grad[None],
        down_grad[None],
        out_proj_grad,
        query_grad.reshape(tokens_here, -1).astype(bf16),
        key_grad.reshape(tokens_here, -1).astype(bf16),
        value_grad.reshape(tokens_here, -1).astype(bf16),
    )


def solution(mesh):
    placed = (
        P("sp", None),
        P("sp", "tp"),
        P("sp", None),
        P("sp", None),
        P("sp", None, "tp"),
        P("sp", None, "tp"),
        P("sp", "tp", None),
        P("tp", None),
        P("sp", "tp"),
        P("sp", "tp"),
        P("sp", "tp"),
        P("sp", "tp"),
        P("sp", "tp"),
        P("sp", "tp", None, None),
    )
    return jax.shard_map(
        on_device,
        mesh=mesh,
        in_specs=placed,
        out_specs=(
            P("sp", None, "tp"),
            P("sp", None, "tp"),
            P("sp", "tp", None),
            P("sp", "tp"),
            P("sp", "tp"),
            P("sp", "tp"),
            P("sp", "tp"),
        ),
        check_vma=False,
    )
```
